32 devices in a mesh: kv: 4 (over y, x), tp: 8 (over z, core).
Axes of the slice: x: 2, y: 2, z: 4, core: 2. Of those that a mesh axis runs over, the one named last changes fastest.
Arguments:
- resid: bfloat16 [32, 4096], P('tp', 'kv'), may hold values from -35 to 35
- attn_gain: bfloat16 [4096], replicated, may hold values from 0.099609375 to 1.8984375
- w_query_nope: bfloat16 [4096, 8192], P('kv', 'tp'), may hold values from -0.09375 to 0.09375
- w_query_rope: bfloat16 [4096, 4096], P('kv', 'tp'), may hold values from -0.09375 to 0.09375
- w_latent: bfloat16 [4096, 512], P('kv'), may hold values from -0.09375 to 0.09375
- w_key_rope: bfloat16 [4096, 64], replicated, may hold values from -0.09375 to 0.09375
- latent_gain: bfloat16 [512], replicated, may hold values from 0.099609375 to 1.8984375
- key_up: bfloat16 [512, 64, 128], P(None, 'tp'), may hold values from -0.5 to 0.5
- value_up: bfloat16 [512, 64, 128], P(None, 'tp'), may hold values from -0.25 to 0.25
- w_out: bfloat16 [8192, 4096], P('tp', 'kv'), may hold values from -4 to 4
- post_gain: bfloat16 [4096], replicated, may hold values from 0.099609375 to 1.8984375
- mlp_gain: bfloat16 [4096], replicated, may hold values from 0.099609375 to 1.8984375
- w_gate: bfloat16 [4096, 11008], P('kv', 'tp'), may hold values from -3 to 3
- w_up: bfloat16 [4096, 11008], P('kv', 'tp'), may hold values from -3 to 3
- w_down: bfloat16 [11008, 4096], P('tp', 'kv'), may hold values from -0.0546875 to 0.0546875
- cache_latent: bfloat16 [32, 2048, 512], P('tp', 'kv'), may hold values from -6 to 6
- cache_rope_key: bfloat16 [32, 2048, 64], P('tp', 'kv'), may hold values from -740 to 740
Outputs:
- next_resid: bfloat16 [32, 4096], P('tp', 'kv')
- new_latent: bfloat16 [32, 512], P('tp')
- new_rope_key: bfloat16 [32, 64], P('tp')
The draws below stay inside these ranges and needn't reach their ends.
All inputs are finite; a program needn't handle non-finite values.
Results may differ from the reference program's by a relative error of at most 0.035.
Values may be sent and summed in bfloat16 or wider, within the bound.
A program may use at most 64 MiB of HBM per device.

```python
import jax
import jax.numpy as jnp
from jax import lax

D = 4096
H = 64
NOPE = 128
ROPE = 64
VD = 128
LAT = 512
FF = 11008
POS_DEV = 512
BATCH = 32
CTX = 2048
N_KV = 4


def rising_profile(length, factor):
    place = (jnp.arange(length, dtype=jnp.float32) + 0.5) / length
    profile = jnp.exp(jnp.log(factor) * (place - 0.5))
    return profile / jnp.sqrt(jnp.mean(profile * profile))


def draw_resid(key, part):
    key_base, key_rows = jax.random.split(jax.random.fold_in(key, 101))
    column_pos = jnp.arange(D, dtype=jnp.float32) / D
    column_scale = 0.5 * jnp.exp(jnp.log(4.0) * column_pos)[None, :]
    base_draw = jnp.clip(jax.random.normal(key_base, (BATCH, D), jnp.float32), -6.0, 6.0)
    row_scale = jnp.exp(jax.random.uniform(key_rows, (BATCH, 1), jnp.float32, -0.5, 0.5))
    return (base_draw * column_scale * row_scale).astype(jnp.bfloat16)


def draw_w_out(key, part):
    factor = 6.0
    base_draw = jnp.clip(jax.random.normal(jax.random.fold_in(key, 103), (H * VD, D), jnp.float32), -6.0, 6.0)
    scaled = base_draw * rising_profile(H * VD, factor)[:, None] * rising_profile(D, factor)[None, :]
    return (scaled * (H * VD) ** (-0.5)).astype(jnp.bfloat16)


def rising_rows(key, factor):
    base_draw = jnp.clip(jax.random.normal(key, (D, FF), jnp.float32), -6.0, 6.0)
    return (base_draw * rising_profile(D, factor)[:, None] * D ** (-0.5)).astype(jnp.bfloat16)


def draw_w_gate(key, part):
    factor = 6.0
    return rising_rows(jax.random.fold_in(key, 107), factor)


def draw_w_up(key, part):
    factor = 6.0
    return rising_rows(jax.random.fold_in(key, 109), factor)


def draw_cache_rope_key(key, part):
    key_base = jax.random.fold_in(jax.random.fold_in(key, 113), 0)
    base_draw = jnp.clip(jax.random.normal(key_base, (BATCH, CTX, ROPE), jnp.float32), -6.0, 6.0)
    return base_draw.astype(jnp.bfloat16)


def block_levels(stream_key, shape, cuts, smallest, top_value):
    def one(dim, blocks):
        draws = jax.random.uniform(jax.random.fold_in(jax.random.fold_in(stream_key, 6), dim), (blocks,), jnp.float32, smallest / len(cuts), top_value / len(cuts))
        return jnp.repeat(jnp.exp(draws), shape[dim] // blocks).reshape((-1,) + (1,) * (len(shape) - dim - 1))

    loudness = one(*cuts[0])
    for cut in cuts[1:]:
        loudness = loudness * one(*cut)
    return loudness


def noise(key, shape, width, reach, pieces=(), kind=jnp.bfloat16):
    values = jax.random.normal(key, shape, jnp.float32) * width
    if len(pieces) > 0:
        values = block_levels(key, shape, pieces, -0.22, 0.18) * values
    return jnp.clip(values, min=-reach, max=reach).astype(kind)


def setup_inputs(seed: int = 0) -> dict:
    streams_of = jax.random.split(jax.random.key(seed), 18)
    resid = draw_resid(jax.random.fold_in(streams_of[17], 71), 0)
    attn_gain = jnp.clip(1.0 + 0.18 * jax.random.normal(streams_of[1], (D,), jnp.float32), 0.099609375, 1.8984375).astype(jnp.bfloat16)
    w_query_nope = noise(streams_of[2], (D, H * NOPE), D ** -0.5, 0.09375, ((0, 4), (1, 8)))
    w_query_rope = noise(streams_of[3], (D, H * ROPE), D ** -0.5, 0.09375, ((0, 4), (1, 8)))
    w_latent = noise(streams_of[4], (D, LAT), D ** -0.5, 0.09375, ((0, 4),))
    w_key_rope = noise(streams_of[5], (D, ROPE), D ** -0.5, 0.09375)
    latent_gain = jnp.clip(1.0 + 0.18 * jax.random.normal(streams_of[6], (LAT,), jnp.float32), 0.099609375, 1.8984375).astype(jnp.bfloat16)
    key_up = noise(streams_of[7], (LAT, H, NOPE), NOPE ** -0.5, 0.5, ((1, 8),))
    value_up = noise(streams_of[8], (LAT, H, VD), LAT ** -0.5, 0.25, ((1, 8),))
    w_out = draw_w_out(jax.random.fold_in(streams_of[17], 71), 0)
    post_gain = jnp.clip(1.0 + 0.18 * jax.random.normal(streams_of[10], (D,), jnp.float32), 0.099609375, 1.8984375).astype(jnp.bfloat16)
    mlp_gain = jnp.clip(1.0 + 0.18 * jax.random.normal(streams_of[11], (D,), jnp.float32), 0.099609375, 1.8984375).astype(jnp.bfloat16)
    w_gate = draw_w_gate(jax.random.fold_in(streams_of[17], 71), 0)
    w_up = draw_w_up(jax.random.fold_in(streams_of[17], 71), 0)
    w_down = noise(streams_of[14], (FF, D), FF ** -0.5, 0.0546875, ((0, 8), (1, 4)))
    cache_latent = noise(streams_of[15], (BATCH, CTX, LAT), 1.0, 6.0, ((0, 8), (1, 4)))
    cache_rope_key = draw_cache_rope_key(jax.random.fold_in(streams_of[17], 71), 0)
    return dict(resid=resid, attn_gain=attn_gain, w_query_nope=w_query_nope, w_query_rope=w_query_rope, w_latent=w_latent, w_key_rope=w_key_rope, latent_gain=latent_gain, key_up=key_up, value_up=value_up, w_out=w_out, post_gain=post_gain, mlp_gain=mlp_gain, w_gate=w_gate, w_up=w_up, w_down=w_down, cache_latent=cache_latent, cache_rope_key=cache_rope_key)


EPS = 1e-06
THETA = 10000.0

def rotate(vector, position):
    half_width = vector.shape[-1] // 2
    frequency = THETA ** (-jnp.arange(half_width, dtype=jnp.float32) / half_width)
    angles = jnp.asarray(position, jnp.float32) * frequency
    cos_table, sin_table = (jnp.cos(angles), jnp.sin(angles))
    lower_half, upper_half = (vector[..., :half_width], vector[..., half_width:])
    return jnp.concatenate([lower_half * cos_table - upper_half * sin_table, lower_half * sin_table + upper_half * cos_table], axis=-1)

def reference(resid, attn_gain, w_query_nope, w_query_rope, w_latent, w_key_rope, latent_gain, key_up, value_up, w_out, post_gain, mlp_gain, w_gate, w_up, w_down, cache_latent, cache_rope_key):
    batch_rows = resid.shape[0]
    head_count = key_up.shape[1]
    context = cache_latent.shape[1]
    latent_width = cache_latent.shape[2]
    score_scale = (key_up.shape[2] + cache_rope_key.shape[2]) ** (-0.5)
    resid_float = resid.astype(jnp.float32)
    normed_a = (resid_float * attn_gain.astype(jnp.float32)).astype(jnp.bfloat16)
    scale_in = lax.rsqrt(lax.optimization_barrier(jnp.mean(resid_float * resid_float, axis=1, keepdims=True)) + EPS)
    q_nope = (jnp.dot(normed_a, w_query_nope, preferred_element_type=jnp.float32) * scale_in).astype(jnp.bfloat16)
    q_rope_raw = jnp.dot(normed_a, w_query_rope, preferred_element_type=jnp.float32) * scale_in
    q_rope = rotate(q_rope_raw.reshape(batch_rows, head_count, -1), context).astype(jnp.bfloat16)
    latent_raw = jnp.dot(normed_a, w_latent, preferred_element_type=jnp.float32)
    new_latent = (latent_raw * lax.rsqrt(lax.optimization_barrier(jnp.mean(latent_raw * latent_raw, axis=1, keepdims=True)) + EPS) * latent_gain.astype(jnp.float32)).astype(jnp.bfloat16)
    key_raw = jnp.dot(normed_a, w_key_rope, preferred_element_type=jnp.float32) * scale_in
    new_rope_key = rotate(key_raw, context).astype(jnp.bfloat16)
    q_lat = jnp.einsum('bhd,chd->bhc', q_nope.reshape(batch_rows, head_count, -1).astype(jnp.float32), key_up.astype(jnp.float32)).astype(jnp.bfloat16)

    def attend(item):
        query_lat, query_rope, keys, rope_keys, own_latent, own_rope = item
        scores = (jnp.dot(query_lat, keys.T, preferred_element_type=jnp.float32) + jnp.dot(query_rope, rope_keys.T, preferred_element_type=jnp.float32)) * score_scale
        own_score = (jnp.dot(query_lat, own_latent, preferred_element_type=jnp.float32) + jnp.dot(query_rope, own_rope, preferred_element_type=jnp.float32)) * score_scale
        peak = jnp.maximum(lax.optimization_barrier(jnp.max(scores, axis=1)), own_score)
        probs = jnp.exp(scores - peak[:, None])
        own_prob = jnp.exp(own_score - peak)
        totals = lax.optimization_barrier(jnp.sum(probs, axis=1)) + own_prob
        weights = probs.astype(jnp.bfloat16).reshape(head_count, N_KV, POS_DEV)
        blocks = keys.reshape(N_KV, POS_DEV, latent_width)
        partial_value = jnp.einsum('hjp,jpc->hjc', weights.astype(jnp.float32), blocks.astype(jnp.float32))
        partial_value = partial_value.astype(jnp.bfloat16).astype(jnp.float32)
        summed = lax.optimization_barrier(jnp.sum(partial_value, axis=1)) + own_prob[:, None] * own_latent.astype(jnp.float32)[None, :]
        return (summed / totals[:, None]).astype(jnp.bfloat16)
    o_lat = lax.map(attend, (q_lat, q_rope, cache_latent, cache_rope_key, new_latent, new_rope_key))
    o_heads = jnp.einsum('bhc,che->bhe', o_lat.astype(jnp.float32), value_up.astype(jnp.float32))
    o_heads = o_heads.astype(jnp.bfloat16).reshape(batch_rows, -1)
    attended = jnp.dot(o_heads, w_out, preferred_element_type=jnp.float32)
    post_part = attended * lax.rsqrt(lax.optimization_barrier(jnp.mean(attended * attended, axis=1, keepdims=True)) + EPS) * post_gain.astype(jnp.float32)
    resid_mid = (resid_float + post_part).astype(jnp.bfloat16)
    mid_float = resid_mid.astype(jnp.float32)
    normed_m = (mid_float * mlp_gain.astype(jnp.float32)).astype(jnp.bfloat16)
    scale_mid = lax.rsqrt(lax.optimization_barrier(jnp.mean(mid_float * mid_float, axis=1, keepdims=True)) + EPS)
    gate = jnp.dot(normed_m, w_gate, preferred_element_type=jnp.float32) * scale_mid
    up_part = jnp.dot(normed_m, w_up, preferred_element_type=jnp.float32) * scale_mid
    hidden = (jax.nn.silu(gate) * up_part).astype(jnp.bfloat16)
    next_resid = (mid_float + jnp.dot(hidden, w_down, preferred_element_type=jnp.float32)).astype(jnp.bfloat16)
    return (next_resid, new_latent, new_rope_key)
```

```python
import functools

import jax
import jax.numpy as jnp
import numpy as np
from jax import lax
from jax.experimental import pallas as pl
from jax.experimental.pallas import tpu as pltpu
from jax.sharding import PartitionSpec as P

EPS = 1e-06
THETA = 10000.0


def rotate(vector, position):
    half_width = vector.shape[-1] // 2
    frequency = THETA ** (-jnp.arange(half_width, dtype=jnp.float32) / half_width)
    angles = jnp.asarray(position, jnp.float32) * frequency
    cos_table, sin_table = (jnp.cos(angles), jnp.sin(angles))
    lower_half, upper_half = (vector[..., :half_width], vector[..., half_width:])
    return jnp.concatenate(
        [
            lower_half * cos_table - upper_half * sin_table,
            lower_half * sin_table + upper_half * cos_table,
        ],
        axis=-1,
    )


def body(
    resid,
    attn_gain,
    w_query_nope,
    w_query_rope,
    w_latent,
    w_key_rope,
    latent_gain,
    key_up,
    value_up,
    w_out,
    post_gain,
    mlp_gain,
    w_gate,
    w_up,
    w_down,
    cache_latent,
    cache_rope_key,
):
    kv_count = lax.axis_size("kv")
    kv_index = lax.axis_index("kv")
    tp_index = lax.axis_index("tp")
    own_rows, width_dev = resid.shape
    model_width = width_dev * kv_count
    heads_dev = key_up.shape[1]
    pos_dev = cache_latent.shape[1]
    context = pos_dev * kv_count
    score_scale = (key_up.shape[2] + cache_rope_key.shape[2]) ** (-0.5)
    col_start = kv_index * width_dev
    row_start = tp_index * own_rows

    def block_of(vector):
        return lax.dynamic_slice_in_dim(vector, col_start, width_dev, 0).astype(jnp.float32)[
            None, :
        ]

    gathered = lax.all_gather(resid, "tp", axis=0, tiled=True)
    batch_rows = gathered.shape[0]
    gathered_float = gathered.astype(jnp.float32)
    normed_a = (gathered_float * block_of(attn_gain)).astype(jnp.bfloat16)
    own_normed = lax.dynamic_slice_in_dim(normed_a, row_start, own_rows, 0)
    key_rows = lax.dynamic_slice_in_dim(w_key_rope, col_start, width_dev, 0)
    q_nope_sum, q_rope_sum, latent_sum, key_sum, square_sum = (
        lax.psum(
            jnp.dot(normed_a, w_query_nope, preferred_element_type=jnp.float32).astype(
                jnp.bfloat16
            ),
            "kv",
        ).astype(jnp.float32),
        lax.psum(
            jnp.dot(normed_a, w_query_rope, preferred_element_type=jnp.float32).astype(
                jnp.bfloat16
            ),
            "kv",
        ).astype(jnp.float32),
        lax.psum(
            jnp.dot(own_normed, w_latent, preferred_element_type=jnp.float32).astype(jnp.bfloat16),
            "kv",
        ).astype(jnp.float32),
        lax.psum(
            jnp.dot(own_normed, key_rows, preferred_element_type=jnp.float32).astype(jnp.bfloat16),
            "kv",
        ).astype(jnp.float32),
        lax.psum(
            jnp.sum(gathered_float * gathered_float, axis=1).astype(jnp.bfloat16), "kv"
        ).astype(jnp.float32),
    )
    scale_in = lax.rsqrt(square_sum / model_width + EPS)[:, None]
    own_scale = lax.dynamic_slice_in_dim(scale_in, row_start, own_rows, 0)
    q_nope = (q_nope_sum * scale_in).astype(jnp.bfloat16).reshape(batch_rows, heads_dev, -1)
    q_rope = rotate((q_rope_sum * scale_in).reshape(batch_rows, heads_dev, -1), context).astype(
        jnp.bfloat16
    )
    new_latent = (
        latent_sum
        * lax.rsqrt(jnp.mean(latent_sum * latent_sum, axis=1, keepdims=True) + EPS)
        * latent_gain.astype(jnp.float32)[None, :]
    ).astype(jnp.bfloat16)
    new_rope_key = rotate(key_sum * own_scale, context).astype(jnp.bfloat16)
    q_lat = jnp.einsum("bhd,chd->bhc", q_nope, key_up, preferred_element_type=jnp.float32).astype(
        jnp.bfloat16
    )
    seq_lat, seq_rope = (
        lax.all_to_all(q_lat, "tp", split_axis=0, concat_axis=1, tiled=True),
        lax.all_to_all(q_rope, "tp", split_axis=0, concat_axis=1, tiled=True),
    )
    scores = (
        jnp.einsum("bhc,bpc->bhp", seq_lat, cache_latent, preferred_element_type=jnp.float32)
        + jnp.einsum("bhr,bpr->bhp", seq_rope, cache_rope_key, preferred_element_type=jnp.float32)
    ) * score_scale
    own_score = (
        jnp.einsum("bhc,bc->bh", seq_lat, new_latent, preferred_element_type=jnp.float32)
        + jnp.einsum("bhr,br->bh", seq_rope, new_rope_key, preferred_element_type=jnp.float32)
    ) * score_scale
    local_peak = jnp.maximum(jnp.max(scores, axis=2), own_score)
    peak = lax.pmax(local_peak, "kv")
    probs = jnp.exp(scores - peak[:, :, None])
    own_prob = jnp.exp(own_score - peak)
    totals = lax.psum(jnp.sum(probs, axis=2), "kv") + own_prob
    partial_value = jnp.einsum(
        "bhp,bpc->bhc", probs.astype(jnp.bfloat16), cache_latent, preferred_element_type=jnp.float32
    )
    summed = (
        lax.psum(partial_value.astype(jnp.bfloat16), "kv").astype(jnp.float32)
        + own_prob[:, :, None] * new_latent.astype(jnp.float32)[:, None, :]
    )
    o_lat = (summed / totals[:, :, None]).astype(jnp.bfloat16)
    head_lat = lax.all_to_all(o_lat, "tp", split_axis=1, concat_axis=0, tiled=True)
    o_heads = jnp.einsum(
        "bhc,che->bhe", head_lat, value_up, preferred_element_type=jnp.float32
    ).astype(jnp.bfloat16)
    o_flat = o_heads.reshape(batch_rows, -1)
    attended = lax.psum_scatter(
        jnp.dot(o_flat, w_out, preferred_element_type=jnp.float32).astype(jnp.bfloat16),
        "tp",
        scatter_dimension=0,
        tiled=True,
    ).astype(jnp.float32)
    post_square = lax.psum(jnp.sum(attended * attended, axis=1), "kv")
    post_part = attended * lax.rsqrt(post_square / model_width + EPS)[:, None] * block_of(post_gain)
    resid_mid = (resid.astype(jnp.float32) + post_part).astype(jnp.bfloat16)
    mid_rows = lax.all_gather(resid_mid, "tp", axis=0, tiled=True)
    mid_float = mid_rows.astype(jnp.float32)
    normed_m = (mid_float * block_of(mlp_gain)).astype(jnp.bfloat16)
    gate_part = jnp.dot(normed_m, w_gate, preferred_element_type=jnp.float32)
    up_part = jnp.dot(normed_m, w_up, preferred_element_type=jnp.float32)
    square_part = jnp.sum(mid_float * mid_float, axis=1)
    gate_sum, up_sum, mid_square = (
        lax.psum(gate_part.astype(jnp.bfloat16), "kv").astype(jnp.float32),
        lax.psum(up_part.astype(jnp.bfloat16), "kv").astype(jnp.float32),
        lax.psum(square_part.astype(jnp.bfloat16), "kv").astype(jnp.float32),
    )
    scale_mid = lax.rsqrt(mid_square / model_width + EPS)[:, None]
    hidden = (jax.nn.silu(gate_sum * scale_mid) * (up_sum * scale_mid)).astype(jnp.bfloat16)
    lowered = lax.psum_scatter(
        jnp.dot(hidden, w_down, preferred_element_type=jnp.float32).astype(jnp.bfloat16),
        "tp",
        scatter_dimension=0,
        tiled=True,
    ).astype(jnp.float32)
    next_resid = (resid_mid.astype(jnp.float32) + lowered).astype(jnp.bfloat16)
    return (next_resid, new_latent, new_rope_key)


F32 = jnp.float32
BF16 = jnp.bfloat16
MESH = pl.DeviceIdType.MESH


def dot_nt(a, b):
    return lax.dot_general(a, b, (((1,), (1,)), ((), ())), preferred_element_type=F32)


def lane_iota(shape):
    return lax.broadcasted_iota(jnp.int32, shape, len(shape) - 1)


def turn(v, cos, sin, half):
    width = v.shape[-1]
    low = lane_iota(v.shape) % (2 * half) < half
    swapped = jnp.where(low, pltpu.roll(v, width - half, 1), pltpu.roll(v, half, 1))
    return v * cos + swapped * sin


def layer_kernel(
    K, T, position_count,
    resid, attn_gain, latent_gain, post_gain, mlp_gain, cos_ref, sin_ref,
    h_wqn, h_wqr, h_wlat, h_wkr, h_ku, h_vu, h_wo, h_wg, h_wu, h_wd, h_cl, h_cr,
    out, out_lat, out_key,
    wqn, wqr, wlat, wkr, ku, vu, wo, wg, wu, wd, cl, cr,
    xbuf, xf, qs, qrv, sqs, sqr, lats, latr, qe, qbuf, accs, accr, mls, mlr,
    nls, nks, osend, obuf, ohs, h3, tall, es, er, ab, sqas, sqa, psq, attf, mids,
    gs, us, gr, ur, sqms, sqmr, hb, ls, lr,
    wsem, ssem, rsem,
):
    k = lax.axis_index("kv")
    t = lax.axis_index("tp")
    R, W = resid.shape
    D = W * K
    B = R * T
    LAT = h_wlat.shape[1]
    ROPE = h_wkr.shape[1]
    QN = h_wqn.shape[1]
    QR = h_wqr.shape[1]
    HD = QR // ROPE
    NOPE = QN // HD
    H = HD * T
    VD = h_vu.shape[1] // HD
    half = ROPE // 2
    score_scale = (NOPE + ROPE) ** (-0.5)
    col = pl.ds(pl.multiple_of(k * W, 128), W)

    loads = {}
    pairs = [
        ("qn", h_wqn, wqn), ("qr", h_wqr, wqr), ("lat", h_wlat, wlat),
        ("kr", h_wkr.at[col], wkr), ("ku", h_ku, ku), ("cl", h_cl, cl), ("cr", h_cr, cr),
        ("vu", h_vu, vu), ("wo", h_wo, wo), ("wg", h_wg, wg), ("wu", h_wu, wu), ("wd", h_wd, wd),
    ]
    for i, (name, src, dst) in enumerate(pairs):
        loads[name] = pltpu.make_async_copy(src, dst, wsem.at[i])
        loads[name].start()

    others = [(a, b) for a in range(K) for b in range(T) if (a, b) != (0, 0)]
    tps = [(0, b) for b in range(1, T)]
    kvs = [(a, 0) for a in range(1, K)]

    def peer(off):
        return lax.rem(k + off[0], K), lax.rem(t + off[1], T)

    barrier = pltpu.get_barrier_semaphore()
    for off in others:
        pl.semaphore_signal(barrier, inc=1, device_id=peer(off), device_id_type=MESH)

    sent = []

    def send(src, dst, off):
        i = len(sent)
        copy = pltpu.make_async_remote_copy(
            src_ref=src, dst_ref=dst, send_sem=ssem.at[i], recv_sem=rsem.at[i],
            device_id=peer(off), device_id_type=MESH,
        )
        copy.start()
        sent.append(copy)
        return copy

    def arrive(copies):
        for copy in copies:
            copy.wait_recv()

    def dot(a, b):
        return jnp.dot(a, b[...], preferred_element_type=F32)

    def put_rows(ref, s, v):
        for c in range(ref.shape[0]):
            ref[c, pl.ds(s, R, stride=T), :] = v[:, c * 128:(c + 1) * 128]

    def rows(ref, s):
        return jnp.concatenate(
            [ref[c, pl.ds(s, R, stride=T), :] for c in range(ref.shape[0])], axis=1
        )

    def put_all(ref, v):
        for c in range(ref.shape[0]):
            ref[c] = v[:, c * 128:(c + 1) * 128]

    def all_rows(ref):
        return jnp.concatenate([ref[c] for c in range(ref.shape[0])], axis=1)

    pl.semaphore_wait(barrier, len(others))

    copies = [send(resid, xbuf.at[t], off) for off in tps]
    xo = resid[...].astype(F32)
    xbuf[pl.ds(t, 1)] = resid[...][None]
    again = attn_gain[:, col].astype(F32)
    own_normed = (xo * again).astype(BF16)
    loads["lat"].wait()
    loads["kr"].wait()
    lats[:, :LAT] = dot(own_normed, wlat)
    lats[:, LAT:LAT + ROPE] = dot(own_normed, wkr)
    lats[:, LAT + ROPE:] = jnp.broadcast_to(
        jnp.sum(xo * xo, axis=1, keepdims=True), (R, lats.shape[1] - LAT - ROPE)
    )
    latr[pl.ds(k, 1)] = lats[...][None]
    lat_copies = [send(lats, latr.at[k], off) for off in kvs]
    arrive(copies)
    for s in range(T):
        put_rows(xf, s, xbuf[s].astype(F32))
    x = all_rows(xf)
    normed = (x * again).astype(BF16)
    sqs[...] = jnp.broadcast_to(jnp.sum(x * x, axis=1, keepdims=True), (B, 128)).reshape(K, T, 128)
    loads["qn"].wait()
    qs[:, :, :QN] = dot(normed, wqn).reshape(K, T, QN).astype(BF16)
    loads["qr"].wait()
    qs[:, :, QN:] = dot(normed, wqr).reshape(K, T, QR).astype(BF16)
    copies = []
    for off in kvs:
        to = peer(off)[0]
        copies.append(send(qs.at[to], qrv.at[k], off))
        copies.append(send(sqs.at[to], sqr.at[k], off))
    qrv[pl.ds(k, 1)] = qs[pl.ds(k, 1)]
    sqr[pl.ds(k, 1)] = sqs[pl.ds(k, 1)]

    arrive(lat_copies)
    lat = sum(latr[s] for s in range(K))
    raw = lat[:, :LAT]
    new_lat = (
        raw * lax.rsqrt(jnp.mean(raw * raw, axis=1, keepdims=True) + EPS)
        * latent_gain[...].astype(F32)
    ).astype(BF16)
    own_scale = lax.rsqrt(lat[:, LAT + ROPE:LAT + ROPE + 1] / D + EPS)
    tail = lat[:, LAT:]
    turned = turn(tail * own_scale, cos_ref[:, :tail.shape[1]], sin_ref[:, :tail.shape[1]], half)
    new_key = jnp.where(lane_iota(turned.shape) < ROPE, turned, 0.0).astype(BF16)
    out_lat[...] = new_lat
    out_key[...] = new_key[:, :ROPE]
    nls[...] = new_lat.astype(F32)
    nks[...] = new_key.astype(F32)

    arrive(copies)
    q = sum(qrv[s].astype(F32) for s in range(K))
    scale = lax.rsqrt(sum(sqr[s] for s in range(K))[:, :1] / D + EPS)
    q_nope = (q[:, :QN] * scale).astype(BF16).astype(F32)
    q_rope = turn(q[:, QN:] * scale, cos_ref[...], sin_ref[...], half).astype(BF16).astype(F32)

    def own_head(width, each):
        shape = (HD, width)
        return lane_iota(shape) // each == lax.broadcasted_iota(jnp.int32, shape, 0)

    def spread(v, each):
        mask = own_head(v.shape[1], each)
        return jnp.concatenate(
            [jnp.where(mask, jnp.broadcast_to(v[i:i + 1], mask.shape), 0.0) for i in range(T)], axis=0
        ).astype(BF16)

    RP = qe.shape[2] - LAT
    fold_shape = (QR, RP)
    fold = (
        lax.broadcasted_iota(jnp.int32, fold_shape, 0) % ROPE == lane_iota(fold_shape)
    ).astype(F32).astype(BF16)
    qe[:, :, LAT:] = jnp.dot(
        spread(q_rope, ROPE), fold, preferred_element_type=F32
    ).reshape(T, HD, RP).astype(BF16)
    loads["ku"].wait()
    qe[:, :, :LAT] = dot_nt(spread(q_nope, NOPE), ku[...]).reshape(T, HD, LAT).astype(BF16)
    copies = [send(qe.at[peer(off)[1]], qbuf.at[k, t], off) for off in others]
    qbuf[pl.ds(k, 1), pl.ds(t, 1)] = qe[pl.ds(t, 1)][None]
    loads["cl"].wait()
    loads["cr"].wait()
    arrive(copies)

    copies = []
    for off in kvs + [(0, 0)]:
        b = peer(off)[0]
        qb32 = qbuf[pl.ds(b, 1)][0].astype(F32).reshape(H, LAT + RP)
        qb = qb32.astype(BF16)
        keys = cl[pl.ds(b, 1)][0]
        scores = (
            dot_nt(qb[:, :LAT], keys) + dot_nt(qb[:, LAT:LAT + ROPE], cr[pl.ds(b, 1)][0])
        ) * score_scale
        m = jnp.max(scores, axis=1, keepdims=True)
        p = jnp.exp(scores - m)
        total = jnp.sum(p, axis=1, keepdims=True)
        acc = jnp.dot(p.astype(BF16), keys, preferred_element_type=F32).astype(BF16)
        ml = jnp.where(lane_iota((H, 128)) < 64, m, total)
        if off == (0, 0):
            accr[pl.ds(k, 1)] = acc[None]
            mlr[pl.ds(k, 1)] = ml[None]
        else:
            mls[off[0]] = ml
            accs[off[0]] = acc
            copies.append(send(mls.at[off[0]], mlr.at[k], off))
            copies.append(send(accs.at[off[0]], accr.at[k], off))
    nl = nls[pl.ds(k, 1), :]
    nk = nks[pl.ds(k, 1), :]
    own_score = (
        jnp.sum(qb32[:, :LAT] * nl, axis=1, keepdims=True)
        + jnp.sum(qb32[:, LAT:] * nk, axis=1, keepdims=True)
    ) * score_scale
    arrive(copies)
    peaks = [mlr[s][:, :1] for s in range(K)]
    peak = own_score
    for m in peaks:
        peak = jnp.maximum(peak, m)
    own_prob = jnp.exp(own_score - peak)
    total = own_prob
    summed = own_prob * nl
    for s in range(K):
        w = jnp.exp(peaks[s] - peak)
        total = total + w * mlr[s][:, 64:65]
        summed = summed + w * accr[s].astype(F32)
    osend[...] = (summed / total).reshape(T, HD, LAT).astype(BF16)
    copies = [send(osend.at[peer(off)[1]], obuf.at[t], off) for off in tps]
    obuf[pl.ds(t, 1)] = osend[pl.ds(t, 1)]
    loads["vu"].wait()
    arrive(copies)
    wide = dot(obuf[...].astype(F32).reshape(T * HD, LAT).astype(BF16), vu)
    mask = own_head(HD * VD, VD)
    for i in range(T):
        ohs[i:i + 1, :] = jnp.sum(
            jnp.where(mask, wide[i * HD:(i + 1) * HD], 0.0), axis=0, keepdims=True
        )
    h3[pl.ds(k, 1)] = ohs[...].astype(BF16)[None]
    copies = [send(h3.at[k], h3.at[k], off) for off in kvs]
    loads["wo"].wait()
    arrive(copies)
    put_all(tall, dot(h3[...].astype(F32).reshape(B, HD * VD).astype(BF16), wo))
    for s in range(T):
        es[s] = rows(tall, s).astype(BF16)
    copies = [send(es.at[peer(off)[1]], er.at[t], off) for off in tps]
    er[pl.ds(t, 1)] = es[pl.ds(t, 1)]
    arrive(copies)
    attended = sum(er[s].astype(F32) for s in range(T))
    sqas[...] = jnp.broadcast_to(jnp.sum(attended * attended, axis=1, keepdims=True), (R, 128))
    ab[pl.ds(t, 1)] = attended.astype(BF16)[None]
    copies = [send(sqas, sqa.at[k, t], off) for off in others]
    copies += [send(ab.at[t], ab.at[t], off) for off in tps]
    sqa[pl.ds(k, 1), pl.ds(t, 1)] = sqas[...][None, None]
    arrive(copies)
    for s in range(T):
        put_rows(attf, s, ab[s].astype(F32))
        psq[pl.ds(s, R, stride=T), :] = sum(sqa[j, s] for j in range(K))
    post_scale = lax.rsqrt(psq[...][:, :1] / D + EPS)
    mid = (
        x + all_rows(attf) * post_scale * post_gain[:, col].astype(F32)
    ).astype(BF16).astype(F32)
    put_all(mids, mid)
    normed_m = (mid * mlp_gain[:, col].astype(F32)).astype(BF16)
    sqms[...] = jnp.broadcast_to(
        jnp.sum(mid * mid, axis=1, keepdims=True), (B, 128)
    ).reshape(K, T, 128)
    FD = wg.shape[1]
    loads["wg"].wait()
    gs[...] = dot(normed_m, wg).reshape(K, T, FD).astype(BF16)
    copies = [send(gs.at[peer(off)[0]], gr.at[k], off) for off in kvs]
    copies += [send(sqms.at[peer(off)[0]], sqmr.at[k], off) for off in kvs]
    loads["wu"].wait()
    us[...] = dot(normed_m, wu).reshape(K, T, FD).astype(BF16)
    copies += [send(us.at[peer(off)[0]], ur.at[k], off) for off in kvs]
    gr[pl.ds(k, 1)] = gs[pl.ds(k, 1)]
    ur[pl.ds(k, 1)] = us[pl.ds(k, 1)]
    sqmr[pl.ds(k, 1)] = sqms[pl.ds(k, 1)]
    arrive(copies)
    mid_scale = lax.rsqrt(sum(sqmr[s] for s in range(K))[:, :1] / D + EPS)
    gate = sum(gr[s].astype(F32) for s in range(K)) * mid_scale
    up = sum(ur[s].astype(F32) for s in range(K)) * mid_scale
    hb[pl.ds(k, 1)] = (gate / (1.0 + jnp.exp(-gate)) * up).astype(BF16)[None]
    copies = [send(hb.at[k], hb.at[k], off) for off in kvs]
    loads["wd"].wait()
    arrive(copies)
    put_all(tall, dot(hb[...].astype(F32).reshape(B, FD).astype(BF16), wd))
    for s in range(T):
        ls[s] = rows(tall, s).astype(BF16)
    copies = [send(ls.at[peer(off)[1]], lr.at[t], off) for off in tps]
    lr[pl.ds(t, 1)] = ls[pl.ds(t, 1)]
    mid_own = rows(mids, t)
    arrive(copies)
    lowered = sum(lr[s].astype(F32) for s in range(T))
    out[...] = (mid_own + lowered).astype(BF16)
    for copy in sent:
        copy.wait_send()


def fused(
    resid, attn_gain, w_query_nope, w_query_rope, w_latent, w_key_rope, latent_gain, key_up,
    value_up, w_out, post_gain, mlp_gain, w_gate, w_up, w_down, cache_latent, cache_rope_key,
):
    K = lax.axis_size("kv")
    T = lax.axis_size("tp")
    R, W = resid.shape
    LAT, HD, _ = key_up.shape
    key_flat = key_up.reshape(LAT, -1)
    value_flat = value_up.reshape(LAT, -1)
    ROPE = w_key_rope.shape[1]
    half = ROPE // 2
    context = cache_latent.shape[1] * K
    angle = context * THETA ** (-np.arange(half, dtype=np.float64) / half)
    cos = np.tile(np.cos(angle), 2 * HD)[None].astype(np.float32)
    sin = np.tile(np.concatenate([-np.sin(angle), np.sin(angle)]), HD)[None].astype(np.float32)
    B = R * T
    H = HD * T
    QN, QR, FD, HV = w_query_nope.shape[1], w_query_rope.shape[1], w_gate.shape[1], value_flat.shape[1]
    big = (w_query_nope, w_query_rope, w_latent, w_key_rope, key_flat, value_flat, w_out, w_gate,
           w_up, w_down, cache_latent, cache_rope_key)

    def held(a):
        return pltpu.VMEM((W, ROPE) if a is w_key_rope else a.shape, a.dtype)

    def bf(*shape):
        return pltpu.VMEM(shape, BF16)

    def fl(*shape):
        return pltpu.VMEM(shape, F32)

    LW = LAT + 128
    slabs = fl(W // 128, B, 128)
    scratch = [held(a) for a in big] + [
        bf(T, R, W), slabs, bf(K, T, QN + QR), bf(K, T, QN + QR), fl(K, T, 128), fl(K, T, 128),
        fl(R, LW), fl(K, R, LW), bf(T, HD, LW), bf(K, T, HD, LW), bf(K, H, LAT), bf(K, H, LAT),
        fl(K, H, 128), fl(K, H, 128), fl(R, LAT), fl(R, 128), bf(T, HD, LAT), bf(T, HD, LAT),
        fl(T, HV), bf(K, T, HV), slabs, bf(T, R, W), bf(T, R, W), bf(T, R, W),
        fl(R, 128), fl(K, T, R, 128), fl(B, 128), slabs, slabs,
        bf(K, T, FD), bf(K, T, FD), bf(K, T, FD), bf(K, T, FD), fl(K, T, 128), fl(K, T, 128),
        bf(K, T, FD), bf(T, R, W), bf(T, R, W),
    ]
    count = 10 * (K - 1) + 5 * (T - 1) + 2 * (K * T - 1) + 8
    vmem = pl.BlockSpec(memory_space=pltpu.VMEM)
    hbm = pl.BlockSpec(memory_space=pl.ANY)
    return pl.pallas_call(
        functools.partial(layer_kernel, K, T, context),
        out_shape=(
            jax.ShapeDtypeStruct((R, W), BF16),
            jax.ShapeDtypeStruct((R, LAT), BF16),
            jax.ShapeDtypeStruct((R, ROPE), BF16),
        ),
        in_specs=[vmem] * 7 + [hbm] * len(big),
        out_specs=(vmem, vmem, vmem),
        scratch_shapes=scratch + [
            pltpu.SemaphoreType.DMA((len(big),)),
            pltpu.SemaphoreType.DMA((count,)),
            pltpu.SemaphoreType.DMA((count,)),
        ],
        compiler_params=pltpu.CompilerParams(
            collective_id=0, has_side_effects=True, vmem_limit_bytes=60 * 1024 * 1024
        ),
    )(
        resid, attn_gain[None], latent_gain[None], post_gain[None], mlp_gain[None],
        jnp.asarray(cos), jnp.asarray(sin), *big,
    )


def layer(*args):
    resid, key_up = args[0], args[7]
    kv, tp = lax.axis_size("kv"), lax.axis_size("tp")
    if resid.shape[0] == kv and key_up.shape[1] == 8 and tp == 8 and resid.shape[1] % 128 == 0:
        return fused(*args)
    return body(*args)


def solution(mesh):
    return jax.shard_map(
        layer,
        mesh=mesh,
        in_specs=(
            P("tp", "kv"),
            P(),
            P("kv", "tp"),
            P("kv", "tp"),
            P("kv", None),
            P(),
            P(),
            P(None, "tp", None),
            P(None, "tp", None),
            P("tp", "kv"),
            P(),
            P(),
            P("kv", "tp"),
            P("kv", "tp"),
            P("tp", "kv"),
            P("tp", "kv", None),
            P("tp", "kv", None),
        ),
        out_specs=(P("tp", "kv"), P("tp", None), P("tp", None)),
        check_vma=False,
    )
```

```python
import functools

import jax
import jax.numpy as jnp
import numpy as np
from jax import lax
from jax.experimental import pallas as pl
from jax.experimental.pallas import tpu as pltpu
from jax.sharding import PartitionSpec as P

EPS = 1e-06
THETA = 10000.0


def rotate(vector, position):
    half_width = vector.shape[-1] // 2
    frequency = THETA ** (-jnp.arange(half_width, dtype=jnp.float32) / half_width)
    angles = jnp.asarray(position, jnp.float32) * frequency
    cos_table, sin_table = (jnp.cos(angles), jnp.sin(angles))
    lower_half, upper_half = (vector[..., :half_width], vector[..., half_width:])
    return jnp.concatenate(
        [
            lower_half * cos_table - upper_half * sin_table,
            lower_half * sin_table + upper_half * cos_table,
        ],
        axis=-1,
    )


def body(
    resid,
    attn_gain,
    w_query_nope,
    w_query_rope,
    w_latent,
    w_key_rope,
    latent_gain,
    key_up,
    value_up,
    w_out,
    post_gain,
    mlp_gain,
    w_gate,
    w_up,
    w_down,
    cache_latent,
    cache_rope_key,
):
    kv_count = lax.axis_size("kv")
    kv_index = lax.axis_index("kv")
    tp_index = lax.axis_index("tp")
    own_rows, width_dev = resid.shape
    model_width = width_dev * kv_count
    heads_dev = key_up.shape[1]
    pos_dev = cache_latent.shape[1]
    context = pos_dev * kv_count
    score_scale = (key_up.shape[2] + cache_rope_key.shape[2]) ** (-0.5)
    col_start = kv_index * width_dev
    row_start = tp_index * own_rows

    def block_of(vector):
        return lax.dynamic_slice_in_dim(vector, col_start, width_dev, 0).astype(jnp.float32)[
            None, :
        ]

    gathered = lax.all_gather(resid, "tp", axis=0, tiled=True)
    batch_rows = gathered.shape[0]
    gathered_float = gathered.astype(jnp.float32)
    normed_a = (gathered_float * block_of(attn_gain)).astype(jnp.bfloat16)
    own_normed = lax.dynamic_slice_in_dim(normed_a, row_start, own_rows, 0)
    key_rows = lax.dynamic_slice_in_dim(w_key_rope, col_start, width_dev, 0)
    q_nope_sum, q_rope_sum, latent_sum, key_sum, square_sum = (
        lax.psum(
            jnp.dot(normed_a, w_query_nope, preferred_element_type=jnp.float32).astype(
                jnp.bfloat16
            ),
            "kv",
        ).astype(jnp.float32),
        lax.psum(
            jnp.dot(normed_a, w_query_rope, preferred_element_type=jnp.float32).astype(
                jnp.bfloat16
            ),
            "kv",
        ).astype(jnp.float32),
        lax.psum(
            jnp.dot(own_normed, w_latent, preferred_element_type=jnp.float32).astype(jnp.bfloat16),
            "kv",
        ).astype(jnp.float32),
        lax.psum(
            jnp.dot(own_normed, key_rows, preferred_element_type=jnp.float32).astype(jnp.bfloat16),
            "kv",
        ).astype(jnp.float32),
        lax.psum(
            jnp.sum(gathered_float * gathered_float, axis=1).astype(jnp.bfloat16), "kv"
        ).astype(jnp.float32),
    )
    scale_in = lax.rsqrt(square_sum / model_width + EPS)[:, None]
    own_scale = lax.dynamic_slice_in_dim(scale_in, row_start, own_rows, 0)
    q_nope = (q_nope_sum * scale_in).astype(jnp.bfloat16).reshape(batch_rows, heads_dev, -1)
    q_rope = rotate((q_rope_sum * scale_in).reshape(batch_rows, heads_dev, -1), context).astype(
        jnp.bfloat16
    )
    new_latent = (
        latent_sum
        * lax.rsqrt(jnp.mean(latent_sum * latent_sum, axis=1, keepdims=True) + EPS)
        * latent_gain.astype(jnp.float32)[None, :]
    ).astype(jnp.bfloat16)
    new_rope_key = rotate(key_sum * own_scale, context).astype(jnp.bfloat16)
    q_lat = jnp.einsum("bhd,chd->bhc", q_nope, key_up, preferred_element_type=jnp.float32).astype(
        jnp.bfloat16
    )
    seq_lat, seq_rope = (
        lax.all_to_all(q_lat, "tp", split_axis=0, concat_axis=1, tiled=True),
        lax.all_to_all(q_rope, "tp", split_axis=0, concat_axis=1, tiled=True),
    )
    scores = (
        jnp.einsum("bhc,bpc->bhp", seq_lat, cache_latent, preferred_element_type=jnp.float32)
        + jnp.einsum("bhr,bpr->bhp", seq_rope, cache_rope_key, preferred_element_type=jnp.float32)
    ) * score_scale
    own_score = (
        jnp.einsum("bhc,bc->bh", seq_lat, new_latent, preferred_element_type=jnp.float32)
        + jnp.einsum("bhr,br->bh", seq_rope, new_rope_key, preferred_element_type=jnp.float32)
    ) * score_scale
    local_peak = jnp.maximum(jnp.max(scores, axis=2), own_score)
    peak = lax.pmax(local_peak, "kv")
    probs = jnp.exp(scores - peak[:, :, None])
    own_prob = jnp.exp(own_score - peak)
    totals = lax.psum(jnp.sum(probs, axis=2), "kv") + own_prob
    partial_value = jnp.einsum(
        "bhp,bpc->bhc", probs.astype(jnp.bfloat16), cache_latent, preferred_element_type=jnp.float32
    )
    summed = (
        lax.psum(partial_value.astype(jnp.bfloat16), "kv").astype(jnp.float32)
        + own_prob[:, :, None] * new_latent.astype(jnp.float32)[:, None, :]
    )
    o_lat = (summed / totals[:, :, None]).astype(jnp.bfloat16)
    head_lat = lax.all_to_all(o_lat, "tp", split_axis=1, concat_axis=0, tiled=True)
    o_heads = jnp.einsum(
        "bhc,che->bhe", head_lat, value_up, preferred_element_type=jnp.float32
    ).astype(jnp.bfloat16)
    o_flat = o_heads.reshape(batch_rows, -1)
    attended = lax.psum_scatter(
        jnp.dot(o_flat, w_out, preferred_element_type=jnp.float32).astype(jnp.bfloat16),
        "tp",
        scatter_dimension=0,
        tiled=True,
    ).astype(jnp.float32)
    post_square = lax.psum(jnp.sum(attended * attended, axis=1), "kv")
    post_part = attended * lax.rsqrt(post_square / model_width + EPS)[:, None] * block_of(post_gain)
    resid_mid = (resid.astype(jnp.float32) + post_part).astype(jnp.bfloat16)
    mid_rows = lax.all_gather(resid_mid, "tp", axis=0, tiled=True)
    mid_float = mid_rows.astype(jnp.float32)
    normed_m = (mid_float * block_of(mlp_gain)).astype(jnp.bfloat16)
    gate_part = jnp.dot(normed_m, w_gate, preferred_element_type=jnp.float32)
    up_part = jnp.dot(normed_m, w_up, preferred_element_type=jnp.float32)
    square_part = jnp.sum(mid_float * mid_float, axis=1)
    gate_sum, up_sum, mid_square = (
        lax.psum(gate_part.astype(jnp.bfloat16), "kv").astype(jnp.float32),
        lax.psum(up_part.astype(jnp.bfloat16), "kv").astype(jnp.float32),
        lax.psum(square_part.astype(jnp.bfloat16), "kv").astype(jnp.float32),
    )
    scale_mid = lax.rsqrt(mid_square / model_width + EPS)[:, None]
    hidden = (jax.nn.silu(gate_sum * scale_mid) * (up_sum * scale_mid)).astype(jnp.bfloat16)
    lowered = lax.psum_scatter(
        jnp.dot(hidden, w_down, preferred_element_type=jnp.float32).astype(jnp.bfloat16),
        "tp",
        scatter_dimension=0,
        tiled=True,
    ).astype(jnp.float32)
    next_resid = (resid_mid.astype(jnp.float32) + lowered).astype(jnp.bfloat16)
    return (next_resid, new_latent, new_rope_key)


F32 = jnp.float32
BF16 = jnp.bfloat16
MESH = pl.DeviceIdType.MESH


def dot_nt(a, b):
    return lax.dot_general(a, b, (((1,), (1,)), ((), ())), preferred_element_type=F32)


def lane_iota(shape):
    return lax.broadcasted_iota(jnp.int32, shape, len(shape) - 1)


def turn(v, cos, sin, half):
    width = v.shape[-1]
    low = lane_iota(v.shape) % (2 * half) < half
    swapped = jnp.where(low, pltpu.roll(v, width - half, 1), pltpu.roll(v, half, 1))
    return v * cos + swapped * sin


def layer_kernel(
    K, T, position_count,
    resid, attn_gain, latent_gain, post_gain, mlp_gain, cos_ref, sin_ref,
    h_wqn, h_wqr, h_wlat, h_wkr, h_ku, h_vu, h_wo, h_wg, h_wu, h_wd, h_cl, h_cr,
    out, out_lat, out_key,
    wqn, wqr, wlat, wkr, ku, vu, wo, wg, wu, wd, cl, cr,
    xbuf, xf, qs, qrv, sqs, sqr, lats, latr, qe, qbuf, accs, accr, mls, mlr,
    nls, nks, osend, obuf, ohs, h3, tall, es, er, ab, sqas, sqa, psq, attf, mids,
    gs, us, gr, ur, sqms, sqmr, hb, ls, lr, wide_ref, kus, vus,
    wsem, ssem, rsem,
):
    k = lax.axis_index("kv")
    t = lax.axis_index("tp")
    R, W = resid.shape
    D = W * K
    B = R * T
    LAT = h_wlat.shape[1]
    ROPE = h_wkr.shape[0]
    QN = h_wqn.shape[1]
    QR = h_wqr.shape[1]
    HD = QR // ROPE
    NOPE = QN // HD
    H = HD * T
    VD = h_vu.shape[1]
    half = ROPE // 2
    score_scale = (NOPE + ROPE) ** (-0.5)
    col = pl.ds(pl.multiple_of(k * W, 128), W)

    loads = {}
    pairs = [
        ("lat", h_wlat, wlat), ("kr", h_wkr.at[:, col], wkr), ("ku", h_ku, ku),
        ("qn", h_wqn, wqn), ("qr", h_wqr, wqr), ("vu", h_vu, vu), ("cl", h_cl, cl), ("cr", h_cr, cr),
        ("wo", h_wo, wo), ("wg", h_wg, wg), ("wu", h_wu, wu), ("wd", h_wd, wd),
    ]
    for i, (name, src, dst) in enumerate(pairs):
        loads[name] = pltpu.make_async_copy(src, dst, wsem.at[i])
        loads[name].start()

    others = [(a, b) for a in range(K) for b in range(T) if (a, b) != (0, 0)]
    tps = [(0, b) for b in range(1, T)]
    kvs = [(a, 0) for a in range(1, K)]

    def peer(off):
        return lax.rem(k + off[0], K), lax.rem(t + off[1], T)

    barrier = pltpu.get_barrier_semaphore()
    for off in others:
        pl.semaphore_signal(barrier, inc=1, device_id=peer(off), device_id_type=MESH)

    sent = []

    def send(src, dst, off):
        i = len(sent)
        copy = pltpu.make_async_remote_copy(
            src_ref=src, dst_ref=dst, send_sem=ssem.at[i], recv_sem=rsem.at[i],
            device_id=peer(off), device_id_type=MESH,
        )
        copy.start()
        sent.append(copy)
        return copy

    def arrive(copies):
        for copy in copies:
            copy.wait_recv()

    def dot(a, b):
        return jnp.dot(a, b[...], preferred_element_type=F32)

    def put_rows(ref, s, v):
        for c in range(ref.shape[0]):
            ref[c, pl.ds(s, R, stride=T), :] = v[:, c * 128:(c + 1) * 128]

    def rows(ref, s):
        return jnp.concatenate(
            [ref[c, pl.ds(s, R, stride=T), :] for c in range(ref.shape[0])], axis=1
        )

    def put_all(ref, v):
        for c in range(ref.shape[0]):
            ref[c] = v[:, c * 128:(c + 1) * 128]

    def all_rows(ref):
        return jnp.concatenate([ref[c] for c in range(ref.shape[0])], axis=1)

    gain_start = pl.multiple_of(k * (W // 128), W // 128)

    def gain_row(g):
        g = g.astype(F32)
        return jnp.concatenate([g[i:i + 1] for i in range(g.shape[0])], axis=1)

    def by_head(src, dst):
        n = src.shape[1]
        wide_ref[...] = src[...].astype(F32)
        for h in range(HD):
            dst[:, h * n:(h + 1) * n] = wide_ref[pl.ds(h, LAT, stride=HD), :].astype(BF16)

    pl.semaphore_wait(barrier, len(others))

    copies = [send(resid, xbuf.at[t], off) for off in tps]
    xo = resid[...].astype(F32)
    xbuf[pl.ds(t, 1)] = resid[...][None]
    again = gain_row(attn_gain[pl.ds(gain_start, W // 128), :])
    own_normed = (xo * again).astype(BF16)
    loads["lat"].wait()
    loads["kr"].wait()
    lats[:, :LAT] = dot(own_normed, wlat)
    lats[:, LAT:LAT + ROPE] = dot_nt(own_normed, wkr[...])
    lats[:, LAT + ROPE:] = jnp.broadcast_to(
        jnp.sum(xo * xo, axis=1, keepdims=True), (R, lats.shape[1] - LAT - ROPE)
    )
    latr[pl.ds(k, 1)] = lats[...][None]
    lat_copies = [send(lats, latr.at[k], off) for off in kvs]
    loads["ku"].wait()
    by_head(ku, kus)
    arrive(copies)
    for s in range(T):
        put_rows(xf, s, xbuf[s].astype(F32))
    x = all_rows(xf)
    normed = (x * again).astype(BF16)
    sqs[...] = jnp.broadcast_to(jnp.sum(x * x, axis=1, keepdims=True), (B, 128)).reshape(K, T, 128)
    loads["qn"].wait()
    qs[:, :, :QN] = dot(normed, wqn).reshape(K, T, QN).astype(BF16)
    loads["qr"].wait()
    qs[:, :, QN:] = dot(normed, wqr).reshape(K, T, QR).astype(BF16)
    copies = []
    for off in kvs:
        to = peer(off)[0]
        copies.append(send(qs.at[to], qrv.at[k], off))
        copies.append(send(sqs.at[to], sqr.at[k], off))
    qrv[pl.ds(k, 1)] = qs[pl.ds(k, 1)]
    sqr[pl.ds(k, 1)] = sqs[pl.ds(k, 1)]

    arrive(lat_copies)
    lat = sum(latr[s] for s in range(K))
    raw = lat[:, :LAT]
    new_lat = (
        raw * lax.rsqrt(jnp.mean(raw * raw, axis=1, keepdims=True) + EPS)
        * gain_row(latent_gain[...])
    ).astype(BF16)
    own_scale = lax.rsqrt(lat[:, LAT + ROPE:LAT + ROPE + 1] / D + EPS)
    tail = lat[:, LAT:]
    turned = turn(tail * own_scale, cos_ref[:, :tail.shape[1]], sin_ref[:, :tail.shape[1]], half)
    new_key = jnp.where(lane_iota(turned.shape) < ROPE, turned, 0.0).astype(BF16)
    out_lat[...] = new_lat
    out_key[...] = new_key[:, :ROPE]
    nls[...] = new_lat.astype(F32)
    nks[...] = new_key.astype(F32)

    arrive(copies)
    q = sum(qrv[s].astype(F32) for s in range(K))
    scale = lax.rsqrt(sum(sqr[s] for s in range(K))[:, :1] / D + EPS)
    q_nope = (q[:, :QN] * scale).astype(BF16).astype(F32)
    q_rope = turn(q[:, QN:] * scale, cos_ref[...], sin_ref[...], half).astype(BF16).astype(F32)

    def own_head(width, each):
        shape = (HD, width)
        return lane_iota(shape) // each == lax.broadcasted_iota(jnp.int32, shape, 0)

    def spread(v, each):
        mask = own_head(v.shape[1], each)
        return jnp.concatenate(
            [jnp.where(mask, jnp.broadcast_to(v[i:i + 1], mask.shape), 0.0) for i in range(T)], axis=0
        ).astype(BF16)

    RP = qe.shape[2] - LAT
    fold_shape = (QR, RP)
    fold = (
        lax.broadcasted_iota(jnp.int32, fold_shape, 0) % ROPE == lane_iota(fold_shape)
    ).astype(F32).astype(BF16)
    qe[:, :, LAT:] = jnp.dot(
        spread(q_rope, ROPE), fold, preferred_element_type=F32
    ).reshape(T, HD, RP).astype(BF16)
    qe[:, :, :LAT] = dot_nt(spread(q_nope, NOPE), kus[...]).reshape(T, HD, LAT).astype(BF16)
    copies = [send(qe.at[peer(off)[1]], qbuf.at[k, t], off) for off in others]
    qbuf[pl.ds(k, 1), pl.ds(t, 1)] = qe[pl.ds(t, 1)][None]
    loads["vu"].wait()
    by_head(vu, vus)
    loads["cl"].wait()
    loads["cr"].wait()
    arrive(copies)

    copies = []
    for off in kvs + [(0, 0)]:
        b = peer(off)[0]
        qb32 = qbuf[pl.ds(b, 1)][0].astype(F32).reshape(H, LAT + RP)
        qb = qb32.astype(BF16)
        keys = cl[pl.ds(b, 1)][0]
        scores = (
            dot_nt(qb[:, :LAT], keys) + jnp.dot(
                qb[:, LAT:LAT + ROPE], cr[pl.ds(b, 1)][0], preferred_element_type=F32
            )
        ) * score_scale
        m = jnp.max(scores, axis=1, keepdims=True)
        p = jnp.exp(scores - m)
        total = jnp.sum(p, axis=1, keepdims=True)
        acc = jnp.dot(p.astype(BF16), keys, preferred_element_type=F32).astype(BF16)
        ml = jnp.where(lane_iota((H, 128)) < 64, m, total)
        if off == (0, 0):
            accr[pl.ds(k, 1)] = acc[None]
            mlr[pl.ds(k, 1)] = ml[None]
        else:
            mls[off[0]] = ml
            accs[off[0]] = acc
            copies.append(send(mls.at[off[0]], mlr.at[k], off))
            copies.append(send(accs.at[off[0]], accr.at[k], off))
    nl = nls[pl.ds(k, 1), :]
    nk = nks[pl.ds(k, 1), :]
    own_score = (
        jnp.sum(qb32[:, :LAT] * nl, axis=1, keepdims=True)
        + jnp.sum(qb32[:, LAT:] * nk, axis=1, keepdims=True)
    ) * score_scale
    arrive(copies)
    peaks = [mlr[s][:, :1] for s in range(K)]
    peak = own_score
    for m in peaks:
        peak = jnp.maximum(peak, m)
    own_prob = jnp.exp(own_score - peak)
    total = own_prob
    summed = own_prob * nl
    for s in range(K):
        w = jnp.exp(peaks[s] - peak)
        total = total + w * mlr[s][:, 64:65]
        summed = summed + w * accr[s].astype(F32)
    osend[...] = (summed / total).reshape(T, HD, LAT).astype(BF16)
    copies = [send(osend.at[peer(off)[1]], obuf.at[t], off) for off in tps]
    obuf[pl.ds(t, 1)] = osend[pl.ds(t, 1)]
    arrive(copies)
    wide = dot(obuf[...].astype(F32).reshape(T * HD, LAT).astype(BF16), vus)
    mask = own_head(HD * VD, VD)
    for i in range(T):
        ohs[i:i + 1, :] = jnp.sum(
            jnp.where(mask, wide[i * HD:(i + 1) * HD], 0.0), axis=0, keepdims=True
        )
    h3[pl.ds(k, 1)] = ohs[...].astype(BF16)[None]
    copies = [send(h3.at[k], h3.at[k], off) for off in kvs]
    loads["wo"].wait()
    arrive(copies)
    put_all(tall, dot(h3[...].astype(F32).reshape(B, HD * VD).astype(BF16), wo))
    for s in range(T):
        es[s] = rows(tall, s).astype(BF16)
    copies = [send(es.at[peer(off)[1]], er.at[t], off) for off in tps]
    er[pl.ds(t, 1)] = es[pl.ds(t, 1)]
    arrive(copies)
    attended = sum(er[s].astype(F32) for s in range(T))
    sqas[...] = jnp.broadcast_to(jnp.sum(attended * attended, axis=1, keepdims=True), (R, 128))
    ab[pl.ds(t, 1)] = attended.astype(BF16)[None]
    copies = [send(sqas, sqa.at[k, t], off) for off in others]
    copies += [send(ab.at[t], ab.at[t], off) for off in tps]
    sqa[pl.ds(k, 1), pl.ds(t, 1)] = sqas[...][None, None]
    arrive(copies)
    for s in range(T):
        put_rows(attf, s, ab[s].astype(F32))
        psq[pl.ds(s, R, stride=T), :] = sum(sqa[j, s] for j in range(K))
    post_scale = lax.rsqrt(psq[...][:, :1] / D + EPS)
    mid = (
        x + all_rows(attf) * post_scale * gain_row(post_gain[pl.ds(gain_start, W // 128), :])
    ).astype(BF16).astype(F32)
    put_all(mids, mid)
    normed_m = (mid * gain_row(mlp_gain[pl.ds(gain_start, W // 128), :])).astype(BF16)
    sqms[...] = jnp.broadcast_to(
        jnp.sum(mid * mid, axis=1, keepdims=True), (B, 128)
    ).reshape(K, T, 128)
    FD = wg.shape[0]
    loads["wg"].wait()
    gs[...] = dot_nt(normed_m, wg[...]).reshape(K, T, FD).astype(BF16)
    copies = [send(gs.at[peer(off)[0]], gr.at[k], off) for off in kvs]
    copies += [send(sqms.at[peer(off)[0]], sqmr.at[k], off) for off in kvs]
    loads["wu"].wait()
    us[...] = dot_nt(normed_m, wu[...]).reshape(K, T, FD).astype(BF16)
    copies += [send(us.at[peer(off)[0]], ur.at[k], off) for off in kvs]
    gr[pl.ds(k, 1)] = gs[pl.ds(k, 1)]
    ur[pl.ds(k, 1)] = us[pl.ds(k, 1)]
    sqmr[pl.ds(k, 1)] = sqms[pl.ds(k, 1)]
    arrive(copies)
    mid_scale = lax.rsqrt(sum(sqmr[s] for s in range(K))[:, :1] / D + EPS)
    gate = sum(gr[s].astype(F32) for s in range(K)) * mid_scale
    up = sum(ur[s].astype(F32) for s in range(K)) * mid_scale
    hb[pl.ds(k, 1)] = (gate / (1.0 + jnp.exp(-gate)) * up).astype(BF16)[None]
    copies = [send(hb.at[k], hb.at[k], off) for off in kvs]
    loads["wd"].wait()
    arrive(copies)
    put_all(tall, dot(hb[...].astype(F32).reshape(B, FD).astype(BF16), wd))
    for s in range(T):
        ls[s] = rows(tall, s).astype(BF16)
    copies = [send(ls.at[peer(off)[1]], lr.at[t], off) for off in tps]
    lr[pl.ds(t, 1)] = ls[pl.ds(t, 1)]
    mid_own = rows(mids, t)
    arrive(copies)
    lowered = sum(lr[s].astype(F32) for s in range(T))
    out[...] = (mid_own + lowered).astype(BF16)
    for copy in sent:
        copy.wait_send()


def fused(
    resid, attn_gain, w_query_nope, w_query_rope, w_latent, w_key_rope, latent_gain, key_up,
    value_up, w_out, post_gain, mlp_gain, w_gate, w_up, w_down, cache_latent, cache_rope_key,
):
    K = lax.axis_size("kv")
    T = lax.axis_size("tp")
    R, W = resid.shape
    LAT, HD, _ = key_up.shape
    key_flat = key_up.reshape(LAT * HD, -1)
    value_flat = value_up.reshape(LAT * HD, -1)
    key_turned, rope_turned = w_key_rope.T, jnp.swapaxes(cache_rope_key, 1, 2)
    gate_turned, up_turned = w_gate.T, w_up.T
    ROPE = w_key_rope.shape[1]
    half = ROPE // 2
    context = cache_latent.shape[1] * K
    angle = context * THETA ** (-np.arange(half, dtype=np.float64) / half)
    cos = np.tile(np.cos(angle), 2 * HD)[None].astype(np.float32)
    sin = np.tile(np.concatenate([-np.sin(angle), np.sin(angle)]), HD)[None].astype(np.float32)
    B = R * T
    H = HD * T
    QN, QR, FD = w_query_nope.shape[1], w_query_rope.shape[1], w_gate.shape[1]
    HV = HD * value_up.shape[2]
    big = (w_query_nope, w_query_rope, w_latent, key_turned, key_flat, value_flat, w_out,
           gate_turned, up_turned, w_down, cache_latent, rope_turned)

    def held(a):
        return pltpu.VMEM((ROPE, W) if a is key_turned else a.shape, a.dtype)

    def bf(*shape):
        return pltpu.VMEM(shape, BF16)

    def fl(*shape):
        return pltpu.VMEM(shape, F32)

    LW = LAT + 128
    slabs = fl(W // 128, B, 128)
    scratch = [held(a) for a in big] + [
        bf(T, R, W), slabs, bf(K, T, QN + QR), bf(K, T, QN + QR), fl(K, T, 128), fl(K, T, 128),
        fl(R, LW), fl(K, R, LW), bf(T, HD, LW), bf(K, T, HD, LW), bf(K, H, LAT), bf(K, H, LAT),
        fl(K, H, 128), fl(K, H, 128), fl(R, LAT), fl(R, 128), bf(T, HD, LAT), bf(T, HD, LAT),
        fl(T, HV), bf(K, T, HV), slabs, bf(T, R, W), bf(T, R, W), bf(T, R, W),
        fl(R, 128), fl(K, T, R, 128), fl(B, 128), slabs, slabs,
        bf(K, T, FD), bf(K, T, FD), bf(K, T, FD), bf(K, T, FD), fl(K, T, 128), fl(K, T, 128),
        bf(K, T, FD), bf(T, R, W), bf(T, R, W),
        fl(*key_flat.shape), bf(LAT, QN), bf(LAT, HV),
    ]
    count = 10 * (K - 1) + 5 * (T - 1) + 2 * (K * T - 1) + 8
    vmem = pl.BlockSpec(memory_space=pltpu.VMEM)
    hbm = pl.BlockSpec(memory_space=pl.ANY)
    return pl.pallas_call(
        functools.partial(layer_kernel, K, T, context),
        out_shape=(
            jax.ShapeDtypeStruct((R, W), BF16),
            jax.ShapeDtypeStruct((R, LAT), BF16),
            jax.ShapeDtypeStruct((R, ROPE), BF16),
        ),
        in_specs=[vmem] * 7 + [hbm] * len(big),
        out_specs=(vmem, vmem, vmem),
        scratch_shapes=scratch + [
            pltpu.SemaphoreType.DMA((len(big),)),
            pltpu.SemaphoreType.DMA((count,)),
            pltpu.SemaphoreType.DMA((count,)),
        ],
        compiler_params=pltpu.CompilerParams(
            collective_id=0, has_side_effects=True, vmem_limit_bytes=60 * 1024 * 1024
        ),
    )(
        resid, *(g.reshape(-1, 128) for g in (attn_gain, latent_gain, post_gain, mlp_gain)),
        jnp.asarray(cos), jnp.asarray(sin), *big,
    )


def layer(*args):
    resid, key_up = args[0], args[7]
    kv, tp = lax.axis_size("kv"), lax.axis_size("tp")
    if resid.shape[0] == kv and key_up.shape[1] == 8 and tp == 8 and resid.shape[1] % 128 == 0:
        return fused(*args)
    return body(*args)


def solution(mesh):
    return jax.shard_map(
        layer,
        mesh=mesh,
        in_specs=(
            P("tp", "kv"),
            P(),
            P("kv", "tp"),
            P("kv", "tp"),
            P("kv", None),
            P(),
            P(),
            P(None, "tp", None),
            P(None, "tp", None),
            P("tp", "kv"),
            P(),
            P(),
            P("kv", "tp"),
            P("kv", "tp"),
            P("tp", "kv"),
            P("tp", "kv", None),
            P("tp", "kv", None),
        ),
        out_specs=(P("tp", "kv"), P("tp", None), P("tp", None)),
        check_vma=False,
    )
```

```python
import functools

import jax
import jax.numpy as jnp
import numpy as np
from jax import lax
from jax.experimental import pallas as pl
from jax.experimental.pallas import tpu as pltpu
from jax.sharding import PartitionSpec as P

EPS = 1e-06
THETA = 10000.0


def rotate(vector, position):
    half_width = vector.shape[-1] // 2
    frequency = THETA ** (-jnp.arange(half_width, dtype=jnp.float32) / half_width)
    angles = jnp.asarray(position, jnp.float32) * frequency
    cos_table, sin_table = (jnp.cos(angles), jnp.sin(angles))
    lower_half, upper_half = (vector[..., :half_width], vector[..., half_width:])
    return jnp.concatenate(
        [
            lower_half * cos_table - upper_half * sin_table,
            lower_half * sin_table + upper_half * cos_table,
        ],
        axis=-1,
    )


def body(
    resid,
    attn_gain,
    w_query_nope,
    w_query_rope,
    w_latent,
    w_key_rope,
    latent_gain,
    key_up,
    value_up,
    w_out,
    post_gain,
    mlp_gain,
    w_gate,
    w_up,
    w_down,
    cache_latent,
    cache_rope_key,
):
    kv_count = lax.axis_size("kv")
    kv_index = lax.axis_index("kv")
    tp_index = lax.axis_index("tp")
    own_rows, width_dev = resid.shape
    model_width = width_dev * kv_count
    heads_dev = key_up.shape[1]
    pos_dev = cache_latent.shape[1]
    context = pos_dev * kv_count
    score_scale = (key_up.shape[2] + cache_rope_key.shape[2]) ** (-0.5)
    col_start = kv_index * width_dev
    row_start = tp_index * own_rows

    def block_of(vector):
        return lax.dynamic_slice_in_dim(vector, col_start, width_dev, 0).astype(jnp.float32)[
            None, :
        ]

    gathered = lax.all_gather(resid, "tp", axis=0, tiled=True)
    batch_rows = gathered.shape[0]
    gathered_float = gathered.astype(jnp.float32)
    normed_a = (gathered_float * block_of(attn_gain)).astype(jnp.bfloat16)
    own_normed = lax.dynamic_slice_in_dim(normed_a, row_start, own_rows, 0)
    key_rows = lax.dynamic_slice_in_dim(w_key_rope, col_start, width_dev, 0)
    q_nope_sum, q_rope_sum, latent_sum, key_sum, square_sum = (
        lax.psum(
            jnp.dot(normed_a, w_query_nope, preferred_element_type=jnp.float32).astype(
                jnp.bfloat16
            ),
            "kv",
        ).astype(jnp.float32),
        lax.psum(
            jnp.dot(normed_a, w_query_rope, preferred_element_type=jnp.float32).astype(
                jnp.bfloat16
            ),
            "kv",
        ).astype(jnp.float32),
        lax.psum(
            jnp.dot(own_normed, w_latent, preferred_element_type=jnp.float32).astype(jnp.bfloat16),
            "kv",
        ).astype(jnp.float32),
        lax.psum(
            jnp.dot(own_normed, key_rows, preferred_element_type=jnp.float32).astype(jnp.bfloat16),
            "kv",
        ).astype(jnp.float32),
        lax.psum(
            jnp.sum(gathered_float * gathered_float, axis=1).astype(jnp.bfloat16), "kv"
        ).astype(jnp.float32),
    )
    scale_in = lax.rsqrt(square_sum / model_width + EPS)[:, None]
    own_scale = lax.dynamic_slice_in_dim(scale_in, row_start, own_rows, 0)
    q_nope = (q_nope_sum * scale_in).astype(jnp.bfloat16).reshape(batch_rows, heads_dev, -1)
    q_rope = rotate((q_rope_sum * scale_in).reshape(batch_rows, heads_dev, -1), context).astype(
        jnp.bfloat16
    )
    new_latent = (
        latent_sum
        * lax.rsqrt(jnp.mean(latent_sum * latent_sum, axis=1, keepdims=True) + EPS)
        * latent_gain.astype(jnp.float32)[None, :]
    ).astype(jnp.bfloat16)
    new_rope_key = rotate(key_sum * own_scale, context).astype(jnp.bfloat16)
    q_lat = jnp.einsum("bhd,chd->bhc", q_nope, key_up, preferred_element_type=jnp.float32).astype(
        jnp.bfloat16
    )
    seq_lat, seq_rope = (
        lax.all_to_all(q_lat, "tp", split_axis=0, concat_axis=1, tiled=True),
        lax.all_to_all(q_rope, "tp", split_axis=0, concat_axis=1, tiled=True),
    )
    scores = (
        jnp.einsum("bhc,bpc->bhp", seq_lat, cache_latent, preferred_element_type=jnp.float32)
        + jnp.einsum("bhr,bpr->bhp", seq_rope, cache_rope_key, preferred_element_type=jnp.float32)
    ) * score_scale
    own_score = (
        jnp.einsum("bhc,bc->bh", seq_lat, new_latent, preferred_element_type=jnp.float32)
        + jnp.einsum("bhr,br->bh", seq_rope, new_rope_key, preferred_element_type=jnp.float32)
    ) * score_scale
    local_peak = jnp.maximum(jnp.max(scores, axis=2), own_score)
    peak = lax.pmax(local_peak, "kv")
    probs = jnp.exp(scores - peak[:, :, None])
    own_prob = jnp.exp(own_score - peak)
    totals = lax.psum(jnp.sum(probs, axis=2), "kv") + own_prob
    partial_value = jnp.einsum(
        "bhp,bpc->bhc", probs.astype(jnp.bfloat16), cache_latent, preferred_element_type=jnp.float32
    )
    summed = (
        lax.psum(partial_value.astype(jnp.bfloat16), "kv").astype(jnp.float32)
        + own_prob[:, :, None] * new_latent.astype(jnp.float32)[:, None, :]
    )
    o_lat = (summed / totals[:, :, None]).astype(jnp.bfloat16)
    head_lat = lax.all_to_all(o_lat, "tp", split_axis=1, concat_axis=0, tiled=True)
    o_heads = jnp.einsum(
        "bhc,che->bhe", head_lat, value_up, preferred_element_type=jnp.float32
    ).astype(jnp.bfloat16)
    o_flat = o_heads.reshape(batch_rows, -1)
    attended = lax.psum_scatter(
        jnp.dot(o_flat, w_out, preferred_element_type=jnp.float32).astype(jnp.bfloat16),
        "tp",
        scatter_dimension=0,
        tiled=True,
    ).astype(jnp.float32)
    post_square = lax.psum(jnp.sum(attended * attended, axis=1), "kv")
    post_part = attended * lax.rsqrt(post_square / model_width + EPS)[:, None] * block_of(post_gain)
    resid_mid = (resid.astype(jnp.float32) + post_part).astype(jnp.bfloat16)
    mid_rows = lax.all_gather(resid_mid, "tp", axis=0, tiled=True)
    mid_float = mid_rows.astype(jnp.float32)
    normed_m = (mid_float * block_of(mlp_gain)).astype(jnp.bfloat16)
    gate_part = jnp.dot(normed_m, w_gate, preferred_element_type=jnp.float32)
    up_part = jnp.dot(normed_m, w_up, preferred_element_type=jnp.float32)
    square_part = jnp.sum(mid_float * mid_float, axis=1)
    gate_sum, up_sum, mid_square = (
        lax.psum(gate_part.astype(jnp.bfloat16), "kv").astype(jnp.float32),
        lax.psum(up_part.astype(jnp.bfloat16), "kv").astype(jnp.float32),
        lax.psum(square_part.astype(jnp.bfloat16), "kv").astype(jnp.float32),
    )
    scale_mid = lax.rsqrt(mid_square / model_width + EPS)[:, None]
    hidden = (jax.nn.silu(gate_sum * scale_mid) * (up_sum * scale_mid)).astype(jnp.bfloat16)
    lowered = lax.psum_scatter(
        jnp.dot(hidden, w_down, preferred_element_type=jnp.float32).astype(jnp.bfloat16),
        "tp",
        scatter_dimension=0,
        tiled=True,
    ).astype(jnp.float32)
    next_resid = (resid_mid.astype(jnp.float32) + lowered).astype(jnp.bfloat16)
    return (next_resid, new_latent, new_rope_key)


F32 = jnp.float32
BF16 = jnp.bfloat16
MESH = pl.DeviceIdType.MESH


def dot_nt(a, b):
    return lax.dot_general(a, b, (((1,), (1,)), ((), ())), preferred_element_type=F32)


def lane_iota(shape):
    return lax.broadcasted_iota(jnp.int32, shape, len(shape) - 1)


def turn(v, cos, sin, half):
    width = v.shape[-1]
    low = lane_iota(v.shape) % (2 * half) < half
    swapped = jnp.where(low, pltpu.roll(v, width - half, 1), pltpu.roll(v, half, 1))
    return v * cos + swapped * sin


def layer_kernel(
    K, T, position_count,
    resid, attn_gain, latent_gain, post_gain, mlp_gain, cos_ref, sin_ref,
    h_wqn, h_wqr, h_wlat, h_wkr, h_ku, h_vu, h_wo, h_wg, h_wu, h_wd, h_cl, h_cr,
    out, out_lat, out_key,
    wqn, wqr, wlat, wkr, ku, vu, wo, wg, wu, wd, cl, cr,
    xbuf, xf, qs, qrv, sqs, sqr, lats, latr, qe, qbuf, accs, accr, mls, mlr,
    nls, nks, osend, obuf, ohs, h3, tall, es, er, ab, sqas, sqa, psq, attf, mids,
    gs, us, gr, ur, sqms, sqmr, hb, ls, lr, wide_ref, kus, vus,
    wsem, ssem, rsem,
):
    k = lax.axis_index("kv")
    t = lax.axis_index("tp")
    R, W = resid.shape
    D = W * K
    B = R * T
    LAT = h_wlat.shape[1]
    ROPE = h_wkr.shape[0]
    QN = h_wqn.shape[1]
    QR = h_wqr.shape[1]
    HD = QR // ROPE
    NOPE = QN // HD
    H = HD * T
    VD = h_vu.shape[1]
    half = ROPE // 2
    score_scale = (NOPE + ROPE) ** (-0.5)
    col = pl.ds(pl.multiple_of(k * W, 128), W)

    loads = {}
    pairs = [
        ("lat", h_wlat, wlat), ("kr", h_wkr.at[:, col], wkr), ("ku", h_ku, ku),
        ("qn", h_wqn, wqn), ("qr", h_wqr, wqr), ("vu", h_vu, vu), ("cl", h_cl, cl), ("cr", h_cr, cr),
        ("wo", h_wo, wo), ("wg", h_wg, wg), ("wu", h_wu, wu), ("wd", h_wd, wd),
    ]
    for i, (name, src, dst) in enumerate(pairs):
        loads[name] = pltpu.make_async_copy(src, dst, wsem.at[i])
        loads[name].start()

    others = [(a, b) for a in range(K) for b in range(T) if (a, b) != (0, 0)]
    tps = [(0, b) for b in range(1, T)]
    kvs = [(a, 0) for a in range(1, K)]

    def peer(off):
        return lax.rem(k + off[0], K), lax.rem(t + off[1], T)

    barrier = pltpu.get_barrier_semaphore()
    for off in others:
        pl.semaphore_signal(barrier, inc=1, device_id=peer(off), device_id_type=MESH)

    sent = []

    def send(src, dst, off):
        i = len(sent)
        copy = pltpu.make_async_remote_copy(
            src_ref=src, dst_ref=dst, send_sem=ssem.at[i], recv_sem=rsem.at[i],
            device_id=peer(off), device_id_type=MESH,
        )
        copy.start()
        sent.append(copy)
        return copy

    def arrive(copies):
        for copy in copies:
            copy.wait_recv()

    def dot(a, b):
        return jnp.dot(a, b[...], preferred_element_type=F32)

    def put_rows(ref, s, v):
        for c in range(ref.shape[0]):
            ref[c, pl.ds(s, R, stride=T), :] = v[:, c * 128:(c + 1) * 128]

    def rows(ref, s):
        return jnp.concatenate(
            [ref[c, pl.ds(s, R, stride=T), :] for c in range(ref.shape[0])], axis=1
        )

    def put_all(ref, v):
        for c in range(ref.shape[0]):
            ref[c] = v[:, c * 128:(c + 1) * 128]

    def all_rows(ref):
        return jnp.concatenate([ref[c] for c in range(ref.shape[0])], axis=1)

    gain_start = pl.multiple_of(k * (W // 128), W // 128)

    def gain_row(g):
        g = g.astype(F32)
        return jnp.concatenate([g[i:i + 1] for i in range(g.shape[0])], axis=1)

    def by_head(src, dst):
        n = src.shape[1]
        wide_ref[...] = src[...].astype(F32)
        for h in range(HD):
            dst[:, h * n:(h + 1) * n] = wide_ref[pl.ds(h, LAT, stride=HD), :].astype(BF16)

    xo = resid[...].astype(F32)
    xbuf[pl.ds(t, 1)] = resid[...][None]
    again = gain_row(attn_gain[pl.ds(gain_start, W // 128), :])
    own_normed = (xo * again).astype(BF16)
    loads["lat"].wait()
    loads["kr"].wait()
    lats[:, :LAT] = dot(own_normed, wlat)
    lats[:, LAT:LAT + ROPE] = dot_nt(own_normed, wkr[...])
    lats[:, LAT + ROPE:] = jnp.broadcast_to(
        jnp.sum(xo * xo, axis=1, keepdims=True), (R, lats.shape[1] - LAT - ROPE)
    )
    latr[pl.ds(k, 1)] = lats[...][None]
    pl.semaphore_wait(barrier, len(others))
    copies = [send(resid, xbuf.at[t], off) for off in tps]
    lat_copies = [send(lats, latr.at[k], off) for off in kvs]
    loads["ku"].wait()
    by_head(ku, kus)
    arrive(copies)
    for s in range(T):
        put_rows(xf, s, xbuf[s].astype(F32))
    x = all_rows(xf)
    normed = (x * again).astype(BF16)
    sqs[...] = jnp.broadcast_to(jnp.sum(x * x, axis=1, keepdims=True), (B, 128)).reshape(K, T, 128)
    loads["qn"].wait()
    qs[:, :, :QN] = dot(normed, wqn).reshape(K, T, QN).astype(BF16)
    loads["qr"].wait()
    qs[:, :, QN:] = dot(normed, wqr).reshape(K, T, QR).astype(BF16)
    copies = []
    for off in kvs:
        to = peer(off)[0]
        copies.append(send(qs.at[to], qrv.at[k], off))
        copies.append(send(sqs.at[to], sqr.at[k], off))
    qrv[pl.ds(k, 1)] = qs[pl.ds(k, 1)]
    sqr[pl.ds(k, 1)] = sqs[pl.ds(k, 1)]

    loads["vu"].wait()
    by_head(vu, vus)
    arrive(lat_copies)
    lat = sum(latr[s] for s in range(K))
    raw = lat[:, :LAT]
    new_lat = (
        raw * lax.rsqrt(jnp.mean(raw * raw, axis=1, keepdims=True) + EPS)
        * gain_row(latent_gain[...])
    ).astype(BF16)
    own_scale = lax.rsqrt(lat[:, LAT + ROPE:LAT + ROPE + 1] / D + EPS)
    tail = lat[:, LAT:]
    turned = turn(tail * own_scale, cos_ref[:, :tail.shape[1]], sin_ref[:, :tail.shape[1]], half)
    new_key = jnp.where(lane_iota(turned.shape) < ROPE, turned, 0.0).astype(BF16)
    out_lat[...] = new_lat
    out_key[...] = new_key[:, :ROPE]
    nls[...] = new_lat.astype(F32)
    nks[...] = new_key.astype(F32)

    arrive(copies)
    q = sum(qrv[s].astype(F32) for s in range(K))
    scale = lax.rsqrt(sum(sqr[s] for s in range(K))[:, :1] / D + EPS)
    q_nope = (q[:, :QN] * scale).astype(BF16).astype(F32)
    q_rope = turn(q[:, QN:] * scale, cos_ref[...], sin_ref[...], half).astype(BF16).astype(F32)

    def own_head(width, each):
        shape = (HD, width)
        return lane_iota(shape) // each == lax.broadcasted_iota(jnp.int32, shape, 0)

    def spread(v, each):
        mask = own_head(v.shape[1], each)
        return jnp.concatenate(
            [jnp.where(mask, jnp.broadcast_to(v[i:i + 1], mask.shape), 0.0) for i in range(T)], axis=0
        ).astype(BF16)

    RP = qe.shape[2] - LAT
    fold_shape = (QR, RP)
    fold = (
        lax.broadcasted_iota(jnp.int32, fold_shape, 0) % ROPE == lane_iota(fold_shape)
    ).astype(F32).astype(BF16)
    qe[:, :, LAT:] = jnp.dot(
        spread(q_rope, ROPE), fold, preferred_element_type=F32
    ).reshape(T, HD, RP).astype(BF16)
    qe[:, :, :LAT] = dot_nt(spread(q_nope, NOPE), kus[...]).reshape(T, HD, LAT).astype(BF16)
    copies = [send(qe.at[peer(off)[1]], qbuf.at[k, t], off) for off in tps]
    relayed = {off: [send(qe.at[t], qbuf.at[k, t], off)] for off in kvs}
    qbuf[pl.ds(k, 1), pl.ds(t, 1)] = qe[pl.ds(t, 1)][None]
    for away, copy in zip(tps, copies):
        copy.wait_recv()
        slot = qbuf.at[k, lax.rem(t + T - away[1], T)]
        for off in kvs:
            relayed[off].append(send(slot, slot, off))
    loads["cl"].wait()
    loads["cr"].wait()

    copies = []
    own_qb = None
    for off in [(0, 0)] + kvs:
        b = peer(off)[0]
        if off != (0, 0):
            arrive(relayed[(K - off[0], 0)])
        qb32 = qbuf[pl.ds(b, 1)][0].astype(F32).reshape(H, LAT + RP)
        qb = qb32.astype(BF16)
        keys = cl[pl.ds(b, 1)][0]
        scores = (
            dot_nt(qb[:, :LAT], keys) + jnp.dot(
                qb[:, LAT:LAT + ROPE], cr[pl.ds(b, 1)][0], preferred_element_type=F32
            )
        ) * score_scale
        m = jnp.max(scores, axis=1, keepdims=True)
        p = jnp.exp(scores - m)
        total = jnp.sum(p, axis=1, keepdims=True)
        acc = jnp.dot(p.astype(BF16), keys, preferred_element_type=F32).astype(BF16)
        ml = jnp.where(lane_iota((H, 128)) < 64, m, total)
        if off == (0, 0):
            own_qb = qb32
            accr[pl.ds(k, 1)] = acc[None]
            mlr[pl.ds(k, 1)] = ml[None]
        else:
            mls[off[0]] = ml
            accs[off[0]] = acc
            copies.append(send(mls.at[off[0]], mlr.at[k], off))
            copies.append(send(accs.at[off[0]], accr.at[k], off))
    nl = nls[pl.ds(k, 1), :]
    nk = nks[pl.ds(k, 1), :]
    own_score = (
        jnp.sum(own_qb[:, :LAT] * nl, axis=1, keepdims=True)
        + jnp.sum(own_qb[:, LAT:] * nk, axis=1, keepdims=True)
    ) * score_scale
    arrive(copies)
    peaks = [mlr[s][:, :1] for s in range(K)]
    peak = own_score
    for m in peaks:
        peak = jnp.maximum(peak, m)
    own_prob = jnp.exp(own_score - peak)
    total = own_prob
    summed = own_prob * nl
    for s in range(K):
        w = jnp.exp(peaks[s] - peak)
        total = total + w * mlr[s][:, 64:65]
        summed = summed + w * accr[s].astype(F32)
    osend[...] = (summed / total).reshape(T, HD, LAT).astype(BF16)
    copies = [send(osend.at[peer(off)[1]], obuf.at[t], off) for off in tps]
    obuf[pl.ds(t, 1)] = osend[pl.ds(t, 1)]
    arrive(copies)
    wide = dot(obuf[...].astype(F32).reshape(T * HD, LAT).astype(BF16), vus)
    mask = own_head(HD * VD, VD)
    for i in range(T):
        ohs[i:i + 1, :] = jnp.sum(
            jnp.where(mask, wide[i * HD:(i + 1) * HD], 0.0), axis=0, keepdims=True
        )
    h3[pl.ds(k, 1)] = ohs[...].astype(BF16)[None]
    copies = [send(h3.at[k], h3.at[k], off) for off in kvs]
    loads["wo"].wait()
    arrive(copies)
    put_all(tall, dot(h3[...].astype(F32).reshape(B, HD * VD).astype(BF16), wo))
    for s in range(T):
        es[s] = rows(tall, s).astype(BF16)
    copies = [send(es.at[peer(off)[1]], er.at[t], off) for off in tps]
    er[pl.ds(t, 1)] = es[pl.ds(t, 1)]
    arrive(copies)
    attended = sum(er[s].astype(F32) for s in range(T))
    sqas[...] = jnp.broadcast_to(jnp.sum(attended * attended, axis=1, keepdims=True), (R, 128))
    ab[pl.ds(t, 1)] = attended.astype(BF16)[None]
    copies = [send(sqas, sqa.at[k, t], off) for off in others]
    copies += [send(ab.at[t], ab.at[t], off) for off in tps]
    sqa[pl.ds(k, 1), pl.ds(t, 1)] = sqas[...][None, None]
    arrive(copies)
    for s in range(T):
        put_rows(attf, s, ab[s].astype(F32))
        psq[pl.ds(s, R, stride=T), :] = sum(sqa[j, s] for j in range(K))
    post_scale = lax.rsqrt(psq[...][:, :1] / D + EPS)
    mid = (
        x + all_rows(attf) * post_scale * gain_row(post_gain[pl.ds(gain_start, W // 128), :])
    ).astype(BF16).astype(F32)
    put_all(mids, mid)
    normed_m = (mid * gain_row(mlp_gain[pl.ds(gain_start, W // 128), :])).astype(BF16)
    sqms[...] = jnp.broadcast_to(
        jnp.sum(mid * mid, axis=1, keepdims=True), (B, 128)
    ).reshape(K, T, 128)
    FD = wg.shape[0]
    loads["wg"].wait()
    gs[...] = dot_nt(normed_m, wg[...]).reshape(K, T, FD).astype(BF16)
    copies = [send(gs.at[peer(off)[0]], gr.at[k], off) for off in kvs]
    copies += [send(sqms.at[peer(off)[0]], sqmr.at[k], off) for off in kvs]
    loads["wu"].wait()
    us[...] = dot_nt(normed_m, wu[...]).reshape(K, T, FD).astype(BF16)
    copies += [send(us.at[peer(off)[0]], ur.at[k], off) for off in kvs]
    gr[pl.ds(k, 1)] = gs[pl.ds(k, 1)]
    ur[pl.ds(k, 1)] = us[pl.ds(k, 1)]
    sqmr[pl.ds(k, 1)] = sqms[pl.ds(k, 1)]
    arrive(copies)
    mid_scale = lax.rsqrt(sum(sqmr[s] for s in range(K))[:, :1] / D + EPS)
    gate = sum(gr[s].astype(F32) for s in range(K)) * mid_scale
    up = sum(ur[s].astype(F32) for s in range(K)) * mid_scale
    hb[pl.ds(k, 1)] = (gate / (1.0 + jnp.exp(-gate)) * up).astype(BF16)[None]
    copies = [send(hb.at[k], hb.at[k], off) for off in kvs]
    loads["wd"].wait()
    arrive(copies)
    put_all(tall, dot(hb[...].astype(F32).reshape(B, FD).astype(BF16), wd))
    for s in range(T):
        ls[s] = rows(tall, s).astype(BF16)
    copies = [send(ls.at[peer(off)[1]], lr.at[t], off) for off in tps]
    lr[pl.ds(t, 1)] = ls[pl.ds(t, 1)]
    mid_own = rows(mids, t)
    arrive(copies)
    lowered = sum(lr[s].astype(F32) for s in range(T))
    out[...] = (mid_own + lowered).astype(BF16)
    for copy in sent:
        copy.wait_send()


def hand_over(a, b, c, a_out, b_out, c_out):
    for src, dst in ((a, a_out), (b, b_out), (c, c_out)):
        dst[...] = src[...]


def fused(
    resid, attn_gain, w_query_nope, w_query_rope, w_latent, w_key_rope, latent_gain, key_up,
    value_up, w_out, post_gain, mlp_gain, w_gate, w_up, w_down, cache_latent, cache_rope_key,
):
    K = lax.axis_size("kv")
    T = lax.axis_size("tp")
    R, W = resid.shape
    LAT, HD, _ = key_up.shape
    key_flat = key_up.reshape(LAT * HD, -1)
    value_flat = value_up.reshape(LAT * HD, -1)
    key_turned, rope_turned = w_key_rope.T, jnp.swapaxes(cache_rope_key, 1, 2)
    gate_turned, up_turned = w_gate.T, w_up.T
    ROPE = w_key_rope.shape[1]
    half = ROPE // 2
    context = cache_latent.shape[1] * K
    angle = context * THETA ** (-np.arange(half, dtype=np.float64) / half)
    cos = np.tile(np.cos(angle), 2 * HD)[None].astype(np.float32)
    sin = np.tile(np.concatenate([-np.sin(angle), np.sin(angle)]), HD)[None].astype(np.float32)
    B = R * T
    H = HD * T
    QN, QR, FD = w_query_nope.shape[1], w_query_rope.shape[1], w_gate.shape[1]
    HV = HD * value_up.shape[2]
    big = (w_query_nope, w_query_rope, w_latent, key_turned, key_flat, value_flat, w_out,
           gate_turned, up_turned, w_down, cache_latent, rope_turned)

    def held(a):
        return pltpu.VMEM((ROPE, W) if a is key_turned else a.shape, a.dtype)

    def bf(*shape):
        return pltpu.VMEM(shape, BF16)

    def fl(*shape):
        return pltpu.VMEM(shape, F32)

    LW = LAT + 128
    slabs = fl(W // 128, B, 128)
    scratch = [held(a) for a in big] + [
        bf(T, R, W), slabs, bf(K, T, QN + QR), bf(K, T, QN + QR), fl(K, T, 128), fl(K, T, 128),
        fl(R, LW), fl(K, R, LW), bf(T, HD, LW), bf(K, T, HD, LW), bf(K, H, LAT), bf(K, H, LAT),
        fl(K, H, 128), fl(K, H, 128), fl(R, LAT), fl(R, 128), bf(T, HD, LAT), bf(T, HD, LAT),
        fl(T, HV), bf(K, T, HV), slabs, bf(T, R, W), bf(T, R, W), bf(T, R, W),
        fl(R, 128), fl(K, T, R, 128), fl(B, 128), slabs, slabs,
        bf(K, T, FD), bf(K, T, FD), bf(K, T, FD), bf(K, T, FD), fl(K, T, 128), fl(K, T, 128),
        bf(K, T, FD), bf(T, R, W), bf(T, R, W),
        fl(*key_flat.shape), bf(LAT, QN), bf(LAT, HV),
    ]
    count = 10 * (K - 1) + 5 * (T - 1) + 2 * (K * T - 1) + 8
    vmem = pl.BlockSpec(memory_space=pltpu.VMEM)
    hbm = pl.BlockSpec(memory_space=pl.ANY)
    out_shape = (
        jax.ShapeDtypeStruct((R, W), BF16),
        jax.ShapeDtypeStruct((R, LAT), BF16),
        jax.ShapeDtypeStruct((R, ROPE), BF16),
    )
    made = pl.pallas_call(
        functools.partial(layer_kernel, K, T, context),
        out_shape=out_shape,
        in_specs=[vmem] * 7 + [hbm] * len(big),
        out_specs=(vmem, vmem, vmem),
        scratch_shapes=scratch + [
            pltpu.SemaphoreType.DMA((len(big),)),
            pltpu.SemaphoreType.DMA((count,)),
            pltpu.SemaphoreType.DMA((count,)),
        ],
        compiler_params=pltpu.CompilerParams(
            collective_id=0, has_side_effects=True, vmem_limit_bytes=60 * 1024 * 1024
        ),
    )(
        resid, *(g.reshape(-1, 128) for g in (attn_gain, latent_gain, post_gain, mlp_gain)),
        jnp.asarray(cos), jnp.asarray(sin), *big,
    )
    return pl.pallas_call(
        hand_over, out_shape=out_shape, in_specs=[vmem] * 3, out_specs=(vmem,) * 3
    )(*made)


def layer(*args):
    resid, key_up = args[0], args[7]
    kv, tp = lax.axis_size("kv"), lax.axis_size("tp")
    if resid.shape[0] == kv and key_up.shape[1] == 8 and tp == 8 and resid.shape[1] % 128 == 0:
        return fused(*args)
    return body(*args)


def solution(mesh):
    return jax.shard_map(
        layer,
        mesh=mesh,
        in_specs=(
            P("tp", "kv"),
            P(),
            P("kv", "tp"),
            P("kv", "tp"),
            P("kv", None),
            P(),
            P(),
            P(None, "tp", None),
            P(None, "tp", None),
            P("tp", "kv"),
            P(),
            P(),
            P("kv", "tp"),
            P("kv", "tp"),
            P("tp", "kv"),
            P("tp", "kv", None),
            P("tp", "kv", None),
        ),
        out_specs=(P("tp", "kv"), P("tp", None), P("tp", None)),
        check_vma=False,
    )
```
